256 devices in a mesh: fs: 32 (over z, x), tp: 8 (over y, core).
Axes of the slice: x: 4, y: 4, z: 8, core: 2. Of those that a mesh axis runs over, the one named last changes fastest.
Arguments:
- tokens: bfloat16 [16384, 2048], P('fs', 'tp'), may hold values from -6 to 6
- pre_gain: float32 [2048], replicated, may hold values from 0.1 to 1.9
- pre_gate: float32 [2048, 2816], P('fs', 'tp'), may hold values from -0.125 to 0.125
- pre_up: float32 [2048, 2816], P('fs', 'tp'), may hold values from -0.125 to 0.125
- pre_down: float32 [2816, 2048], P('fs', 'tp'), may hold values from -0.109375 to 0.109375
- mix_gain: float32 [2048], replicated, may hold values from 0.1 to 1.9
- branch_proj: float32 [2048, 1024], P('fs', 'tp'), may hold values from -0.125 to 0.125
- gate_proj: float32 [2048, 1024], P('fs', 'tp'), may hold values from -0.125 to 0.125
- conv_taps: float32 [4, 1024], P(None, 'tp'), may hold values from -3 to 3
- retain_blocks: float32 [16, 64, 64], P('tp'), may hold values from -0.75 to 0.75
- admit_blocks: float32 [16, 64, 64], P('tp'), may hold values from -0.75 to 0.75
- decay_param: float32 [1024], P('tp'), may hold values from 5 to 8.5
- channel_gain: float32 [1024], replicated, may hold values from 0.1 to 1.9
- out_proj: float32 [1024, 2048], P('fs', 'tp'), may hold values from -0.1875 to 0.1875
- post_gain: float32 [2048], replicated, may hold values from 0.1 to 1.9
- post_gate: float32 [2048, 2816], P('fs', 'tp'), may hold values from -0.125 to 0.125
- post_up: float32 [2048, 2816], P('fs', 'tp'), may hold values from -0.125 to 0.125
- post_down: float32 [2816, 2048], P('fs', 'tp'), may hold values from -0.109375 to 0.109375
Outputs:
- layer_out: bfloat16 [16384, 2048], P('fs', 'tp')
The draws below stay inside these ranges and needn't reach their ends.
All inputs are finite; a program needn't handle non-finite values.
Results may differ from the reference program's by a relative error of at most 0.012.
Values may be sent and summed in bfloat16 or wider, within the bound.
A program may use at most 64 MiB of HBM per device.

```python
import jax
import jax.numpy as jnp
from jax import lax

D = 2048
FF = 2816
HEADS = 16
BLOCK = 64
CONV = 4
SEQ_LEN = 128
DL = 1024
TOKENS = 16384


def block_levels(key, dims, shards, least, largest):
    factor_of = 1.0
    for dim, blocks in shards:
        draws = jax.random.uniform(jax.random.fold_in(jax.random.fold_in(key, 6), dim), (blocks,), jnp.float32, least / len(shards), largest / len(shards))
        factor_of = factor_of * jnp.repeat(jnp.exp(draws), dims[dim] // blocks).reshape((-1,) + (1,) * (len(dims) - 1 - dim))
    return factor_of


def noise(key, shape, scale, bound, cuts=(), held_as=jnp.bfloat16):
    level = block_levels(key, shape, cuts, -0.22, 0.18) if cuts else 1.0
    result = jax.random.normal(key, shape, jnp.float32) * scale * level
    return jnp.minimum(jnp.maximum(result, -bound), bound).astype(held_as)


def setup_inputs(seed: int = 0) -> dict:
    streams_of = jax.random.split(jax.random.key(seed), 19)
    return {
        "tokens": noise(streams_of[0], (TOKENS, D), 1.0, 6.0, ((0, 32), (1, 8))),
        "pre_gain": jnp.clip(1.0 + 0.18 * jax.random.normal(streams_of[1], (D,), jnp.float32), 0.1, 1.9),
        "pre_gate": noise(streams_of[2], (D, FF), D ** -0.5, 0.125, ((0, 32), (1, 8)), jnp.float32),
        "pre_up": noise(streams_of[3], (D, FF), D ** -0.5, 0.125, ((0, 32), (1, 8)), jnp.float32),
        "pre_down": noise(streams_of[4], (FF, D), FF ** -0.5, 0.109375, ((0, 32), (1, 8)), jnp.float32),
        "mix_gain": jnp.clip(1.0 + 0.18 * jax.random.normal(streams_of[5], (D,), jnp.float32), 0.1, 1.9),
        "branch_proj": noise(streams_of[6], (D, DL), D ** -0.5, 0.125, ((0, 32), (1, 8)), jnp.float32),
        "gate_proj": noise(streams_of[7], (D, DL), D ** -0.5, 0.125, ((0, 32), (1, 8)), jnp.float32),
        "conv_taps": noise(streams_of[8], (CONV, DL), CONV ** -0.5, 3.0, ((1, 8),), jnp.float32),
        "retain_blocks": noise(streams_of[9], (HEADS, BLOCK, BLOCK), BLOCK ** -0.5, 0.75, ((0, 8),), jnp.float32),
        "admit_blocks": noise(streams_of[10], (HEADS, BLOCK, BLOCK), BLOCK ** -0.5, 0.75, ((0, 8),), jnp.float32),
        "decay_param": jnp.clip(5.0 + 3.5 * jax.random.uniform(streams_of[11], (DL,), jnp.float32) ** block_levels(streams_of[11], (DL,), ((0, 8),), -0.2, 0.2), 5.0, 8.5),
        "channel_gain": jnp.clip(1.0 + 0.18 * jax.random.normal(streams_of[12], (DL,), jnp.float32), 0.1, 1.9),
        "out_proj": noise(streams_of[13], (DL, D), DL ** -0.5, 0.1875, ((0, 32), (1, 8)), jnp.float32),
        "post_gain": jnp.clip(1.0 + 0.18 * jax.random.normal(streams_of[14], (D,), jnp.float32), 0.1, 1.9),
        "post_gate": noise(streams_of[15], (D, FF), D ** -0.5, 0.125, ((0, 32), (1, 8)), jnp.float32),
        "post_up": noise(streams_of[16], (D, FF), D ** -0.5, 0.125, ((0, 32), (1, 8)), jnp.float32),
        "post_down": noise(streams_of[17], (FF, D), FF ** -0.5, 0.109375, ((0, 32), (1, 8)), jnp.float32),
    }


EPSILON = 1e-06
DECAY_SCALE = 8.0

def normalize(values, norm_gain):
    floats = values.astype(jnp.float32)
    scaled = floats * lax.rsqrt(lax.optimization_barrier(jnp.mean(floats * floats, axis=-1, keepdims=True)) + EPSILON)
    return (scaled * norm_gain).astype(jnp.bfloat16)

def product(operand, matrix):
    return jnp.dot(operand, matrix.astype(jnp.bfloat16), preferred_element_type=jnp.float32)

def combine(earlier, latter):
    keep_early, add_early = earlier
    keep_late, add_late = latter
    return (keep_early * keep_late, keep_late * add_early + add_late)

def feed_forward(residual, norm_gain, gate_matrix, up_matrix, down_matrix):
    normed = normalize(residual, norm_gain)
    hidden = (jax.nn.silu(product(normed, gate_matrix)) * product(normed, up_matrix)).astype(jnp.bfloat16)
    return (residual.astype(jnp.float32) + 0.5 * product(hidden, down_matrix)).astype(jnp.bfloat16)

def block_gate(convolved, blocks):
    rounded = lax.optimization_barrier(blocks.astype(jnp.bfloat16)).astype(jnp.float32)
    grouped = convolved.astype(jnp.float32).reshape(convolved.shape[0], convolved.shape[1], blocks.shape[0], blocks.shape[1])
    mixed = jnp.einsum('sthi,hij->sthj', grouped, rounded)
    return jax.nn.sigmoid(mixed).reshape(convolved.shape)

def recurrent_mixer(residual, norm_gain, branch_matrix, gate_matrix, conv_taps, retain_blocks, admit_blocks, decay_param, channel_gain, out_matrix):
    normed = normalize(residual, norm_gain)
    branch = product(normed, branch_matrix)
    gate_act = product(normed, gate_matrix)
    sequences = residual.shape[0] // SEQ_LEN
    channel_count = branch.shape[1]
    framed = branch.reshape(sequences, SEQ_LEN, channel_count)
    padded = jnp.pad(framed, ((0, 0), (CONV - 1, 0), (0, 0)))
    convolved = jnp.zeros_like(framed)
    for tap_index in range(CONV):
        convolved = convolved + padded[:, tap_index:tap_index + SEQ_LEN] * conv_taps[tap_index]
    convolved = convolved.astype(jnp.bfloat16)
    retained = block_gate(convolved, retain_blocks)
    admitted = block_gate(convolved, admit_blocks)
    log_keep = -DECAY_SCALE * retained * jax.nn.softplus(-decay_param)
    inject = jnp.sqrt(-jnp.expm1(2.0 * log_keep)) * admitted * convolved.astype(jnp.float32)
    _, states = lax.associative_scan(combine, (jnp.exp(log_keep), inject), axis=1)
    mixed_rows = (states.reshape(residual.shape[0], channel_count) * jax.nn.gelu(gate_act)).astype(jnp.bfloat16)
    mixed_normed = normalize(mixed_rows, channel_gain)
    return (residual.astype(jnp.float32) + product(mixed_normed, out_matrix)).astype(jnp.bfloat16)

def reference(tokens, pre_gain, pre_gate, pre_up, pre_down, mix_gain, branch_proj, gate_proj, conv_taps, retain_blocks, admit_blocks, decay_param, channel_gain, out_proj, post_gain, post_gate, post_up, post_down):
    after_pre = feed_forward(tokens, pre_gain, pre_gate, pre_up, pre_down)
    after_mix = recurrent_mixer(after_pre, mix_gain, branch_proj, gate_proj, conv_taps, retain_blocks, admit_blocks, decay_param, channel_gain, out_proj)
    return feed_forward(after_mix, post_gain, post_gate, post_up, post_down)
```

```python
import functools

import jax
import jax.numpy as jnp
from jax import lax
from jax.experimental import pallas as pl
from jax.experimental.pallas import tpu as pltpu
from jax.sharding import Mesh
from jax.sharding import PartitionSpec as P


EPSILON = 1e-06
DECAY_SCALE = 8.0
NZ, NX, NY = 8, 4, 4
TP = 8
SEQ_LEN = 128
ROWS = 512
CHUNKS = ROWS // SEQ_LEN
LANES = 128
BF16, F32 = jnp.bfloat16, jnp.float32
MESH = pl.DeviceIdType.MESH

W1, W2, W3, W4, W5, W6 = "W1", "W2", "W3", "W4", "W5", "W6"
UNIT = {W1: 64, W2: 96, W3: 64, W4: 32, W5: 64, W6: 96}
TILES = {W1: 6, W2: 2, W3: 2, W4: 2, W5: 6, W6: 2}
OFFSET = {}
SLAB = 0
for _name in (W1, W2, W3, W4, W5, W6):
    OFFSET[_name] = SLAB
    SLAB += UNIT[_name] * TILES[_name]

PIECES = (
    (OFFSET[W1], 160, 224, (W1,)),
    (OFFSET[W2], 80, 112, (W2,)),
    (OFFSET[W3], 80, 112, (W3, W4)),
    (OFFSET[W5], 160, 224, (W5,)),
    (OFFSET[W6], 80, 112, (W6,)),
)
PIECE_OF = {W1: 0, W2: 1, W3: 2, W4: 2, W5: 3, W6: 4}
MAX_COPIES = 448

RATE = {"f": 60e3, "b": 33e3, "zf": 50e3, "zb": 40e3, "d": 500e3}
LATENCY = {"link": 2.2, "d": 1.1}
COST = {1: 1.7, 2: 1.0, 3: 1.6, 4: 0.6, 5: 1.7, 6: 1.0}


class Task:
    def __init__(self, name, fn, after=(), needs=(), sends=(), cost=0.05, rank=0):
        self.name, self.fn, self.after, self.needs = name, fn, after, needs
        self.sends, self.cost, self.rank = sends, cost, rank


def ordered(tasks):
    done, arrival, free, now, order = set(), {}, {}, 0.0, []
    left = list(tasks)
    while left:
        best = None
        for task in left:
            if any(a not in done for a in task.after) or any(m not in arrival for m in task.needs):
                continue
            ready = max([arrival[m] for m in task.needs], default=0.0)
            key = (max(ready, now), task.rank, ready)
            if best is None or key < best[0]:
                best = (key, task)
        key, task = best
        now = key[0] + task.cost
        for message, queue, size in task.sends:
            begin = max(free.get(queue, 0.0), now)
            kind = queue if queue in RATE else queue[1]
            end = begin + size / RATE[kind]
            free[queue] = end
            arrival[message] = end + LATENCY["d" if queue == "d" else "link"]
        done.add(task.name)
        left.remove(task)
        order.append(task)
    ordered.estimate = now
    return order


def stable_one_minus_exp(t):
    series = 1.0 - t * (1.0 / 8.0)
    for n in (7.0, 6.0, 5.0, 4.0, 3.0, 2.0):
        series = 1.0 - t * (1.0 / n) * series
    return jnp.where(t < 0.5, t * series, 1.0 - jnp.exp(-t))


def softplus(v):
    e = jnp.exp(-jnp.abs(v))
    u = e / (2.0 + e)
    s = u * u
    total = jnp.zeros_like(s)
    for n in (19, 17, 15, 13, 11, 9, 7, 5, 3, 1):
        total = total * s + 1.0 / n
    return jnp.maximum(v, 0.0) + 2.0 * u * total


def silu(v):
    return v / (1.0 + jnp.exp(-v))


def sigmoid(v):
    return 1.0 / (1.0 + jnp.exp(-v))


def gelu(v):
    return 0.5 * v * (1.0 + jnp.tanh(0.7978845608028654 * (v + 0.044715 * (v * v * v))))


def kernel(
    tokens, pre_gate, pre_up, pre_down, branch_proj, gate_proj, out_proj, post_gate, post_up,
    post_down, pre_gain, mix_gain, channel_gain, post_gain, taps, retain, admit, decay,
    out,
    s_pre_gate, s_pre_up, s_pre_down, s_branch, s_gate, s_out, s_post_gate, s_post_up, s_post_down,
    slab, x1, x2, x3, h1, h2, mixed, wide, spread, blocks, local_sem, send_sem, recv_sem,
):
    z, x, y, c = (lax.axis_index(a) for a in ("z", "x", "y", "c"))
    step = 1 - 2 * c
    me = y * 2 + c

    shards = {
        "pre_gate": (pre_gate, s_pre_gate), "pre_up": (pre_up, s_pre_up),
        "pre_down": (pre_down, s_pre_down), "branch": (branch_proj, s_branch),
        "gate": (gate_proj, s_gate), "out": (out_proj, s_out),
        "post_gate": (post_gate, s_post_gate), "post_up": (post_up, s_post_up),
        "post_down": (post_down, s_post_down),
    }
    loads = {}
    for n, (key, (src, dst)) in enumerate(shards.items()):
        loads[key] = pltpu.make_async_copy(src, dst, local_sem.at[n])
        loads[key].start()
    token_load = pltpu.make_async_copy(tokens, x1.at[me], local_sem.at[len(shards)])
    token_load.start()

    def toward(axis, n, index, distance):
        return {axis: lax.rem(index + distance + n, n)}

    neighbours = [toward(a, n, i, d) for a, n, i in (("z", NZ, z), ("x", NX, x), ("y", NY, y)) for d in (1, -1)]
    neighbours.append({"c": 1 - c})
    barrier = pltpu.get_barrier_semaphore()
    for device in neighbours:
        pl.semaphore_signal(barrier, inc=1, device_id=device, device_id_type=MESH)

    copies = {}

    def send(message, src, dst, device):
        n = len(copies)
        copy = pltpu.make_async_remote_copy(
            src_ref=src, dst_ref=dst, send_sem=send_sem.at[n], recv_sem=recv_sem.at[n],
            device_id=device, device_id_type=MESH,
        )
        copies[message] = copy
        copy.start()

    def arrived(message):
        copies[message].wait_recv()

    lane = lax.broadcasted_iota(jnp.int32, (352, 384), 1)
    row = lax.broadcasted_iota(jnp.int32, (352, 384), 0)
    group = (lane >= 96).astype(jnp.int32) + (lane >= 192).astype(jnp.int32) + (lane >= 288).astype(jnp.int32)
    spread[...] = jnp.where((row == lane - 8 * group) & (lane - 96 * group < 88), 1.0, 0.0).astype(BF16)

    def put(name, tile, value):
        start = OFFSET[name] + UNIT[name] * tile
        slab[z, x, start : start + UNIT[name], :] = value.astype(BF16)

    def build_wide(name, gate_key, up_key):
        for half, key in enumerate((gate_key, up_key)):
            loads[key].wait()
            placed = jnp.dot(shards[key][1][...].astype(BF16), spread[...], preferred_element_type=F32)
            for tile in range(3):
                put(name, half * 3 + tile, placed[:, tile * LANES : (tile + 1) * LANES])

    def build_down(name, key):
        loads[key].wait()
        for tile in range(2):
            value = shards[key][1][:, tile * LANES : (tile + 1) * LANES]
            put(name, tile, jnp.concatenate((value, jnp.zeros((8, LANES), F32)), axis=0))

    def build_mixer():
        loads["branch"].wait()
        put(W3, 0, s_branch[...])
        loads["gate"].wait()
        put(W3, 1, s_gate[...])

    def build_out():
        loads["out"].wait()
        for tile in range(2):
            put(W4, tile, s_out[:, tile * LANES : (tile + 1) * LANES])

    def build_blocks():
        tall = lax.broadcasted_iota(jnp.int32, (LANES, 64), 0)
        flat = lax.broadcasted_iota(jnp.int32, (LANES, 64), 1)
        wide_r = lax.broadcasted_iota(jnp.int32, (64, LANES), 0)
        wide_c = lax.broadcasted_iota(jnp.int32, (64, LANES), 1)
        for n, ref in enumerate((retain, admit)):
            total = jnp.zeros((LANES, LANES), F32)
            for b in range(2):
                left = jnp.where(tall == flat + 64 * b, 1.0, 0.0).astype(BF16)
                right = jnp.where(wide_c == wide_r + 64 * b, 1.0, 0.0).astype(BF16)
                spread_b = jnp.dot(ref[b].astype(BF16), right, preferred_element_type=F32).astype(BF16)
                total = total + jnp.dot(left, spread_b, preferred_element_type=F32)
            blocks[n] = total.astype(BF16)

    builds = {
        W1: lambda: build_wide(W1, "pre_gate", "pre_up"),
        W2: lambda: build_down(W2, "pre_down"),
        W3: build_mixer,
        W4: build_out,
        W5: lambda: build_wide(W5, "post_gate", "post_up"),
        W6: lambda: build_down(W6, "post_down"),
    }

    tasks = []

    def add(*args, **kwargs):
        tasks.append(Task(*args, **kwargs))

    def ring(label, axis, block, size, after, rank):
        n, index = {"x": (NX, x), "z": (NZ, z)}[axis]
        far = n // 2
        near = far - 1
        queue = {"f": axis + "f", "b": axis + "b"}

        def hop(way, k):
            sign = step if way == "f" else -step
            origin = lax.rem(index - sign * (k - 1) + n, n)
            send((label, way, k), block(origin), block(origin), toward(axis, n, index, sign))

        def begin():
            hop("f", 1)
            hop("b", 1)

        add((label, "start"), begin, after=after, rank=rank, cost=0.1,
            sends=[((label, w, 1), queue[w], size) for w in "fb"])
        names = []
        for way, last in (("f", far), ("b", near)):
            previous = (label, "start")
            for k in range(1, last + 1):
                def relay(way=way, k=k, last=last):
                    arrived((label, way, k))
                    if k < last:
                        hop(way, k + 1)
                name = (label, way, k, "relay")
                add(name, relay, after=(previous,), needs=((label, way, k),), rank=rank,
                    sends=[((label, way, k + 1), queue[way], size)] if k < last else [])
                names.append(name)
                previous = name
        return tuple(names)

    piece_done = []
    for p, (first, rows_a, rows_b, needed) in enumerate(PIECES):
        ready = tuple(("build", name) for name in needed)
        for name in needed:
            add(("build", name), builds[name], cost=0.4, rank=p)
        span_a, span_b = slice(first, first + rows_a), slice(first + rows_a, first + rows_a + rows_b)
        size_a, size_b = rows_a * LANES * 2, rows_b * LANES * 2
        a1 = ring((p, "a1"), "x", lambda i, s=span_a: slab.at[z, i, s, :], size_a, ready, p)
        b1 = ring((p, "b1"), "z", lambda i, s=span_b: slab.at[i, x, s, :], size_b, ready, p)
        a2 = ring((p, "a2"), "z", lambda i, s=span_a: slab.at[i, :, s, :], NX * size_a, a1, p)
        b2 = ring((p, "b2"), "x", lambda i, s=span_b: slab.at[:, i, s, :], NZ * size_b, b1, p)
        piece_done.append(a2 + b2)
    for task in tasks:
        if task.name[-1] == "start" and task.name[0][0] > 0 and task.name[0][1] in ("a1", "b1"):
            task.after = task.after + (((task.name[0][0] - 1, task.name[0][1][0] + "2"), "start"),)

    held = {1: (x1, 256), 2: (h1, 384), 3: (x2, 256), 4: (mixed, 128), 5: (x3, 256), 6: (h2, 384)}

    def share(stage, chunk, slot, hops):
        ref = held[stage][0].at[slot, chunk * SEQ_LEN : (chunk + 1) * SEQ_LEN, :]
        for tag, device in hops:
            send((stage, chunk, tag), ref, ref, device)

    up, down, partner = toward("y", NY, y, step), toward("y", NY, y, -step), {"c": 1 - c}

    def slot_at(distance):
        return lax.rem(y + distance + NY, NY) * 2 + c

    def share_own(stage, chunk):
        share(stage, chunk, me, ((("f", 1), up), (("b", 1), down), (("d", 0), partner)))

    def share_tasks(stage, chunk):
        size = SEQ_LEN * held[stage][1] * 2
        rank = -1

        def first():
            arrived((stage, chunk, ("f", 1)))
            share(stage, chunk, slot_at(-step), ((("f", 2), up), (("d", 1), partner)))

        def second():
            arrived((stage, chunk, ("b", 1)))
            share(stage, chunk, slot_at(step), ((("d", 2), partner),))

        def third():
            arrived((stage, chunk, ("f", 2)))
            share(stage, chunk, slot_at(2), ((("d", 3), partner),))

        key = (stage, chunk)
        add((key, "first"), first, needs=((stage, chunk, ("f", 1)),), rank=rank,
            sends=[((stage, chunk, ("f", 2)), "yf", size), ((stage, chunk, ("d", 1)), "d", size)])
        add((key, "second"), second, after=((key, "first"),), needs=((stage, chunk, ("b", 1)),), rank=rank,
            sends=[((stage, chunk, ("d", 2)), "d", size)])
        add((key, "third"), third, after=((key, "second"),), needs=((stage, chunk, ("f", 2)),), rank=rank,
            sends=[((stage, chunk, ("d", 3)), "d", size)])

    def own_sends(stage, chunk):
        size = SEQ_LEN * held[stage][1] * 2
        return [((stage, chunk, ("f", 1)), "yf", size), ((stage, chunk, ("b", 1)), "yb", size),
                ((stage, chunk, ("d", 0)), "d", size)]

    def rows_of(chunk):
        return slice(chunk * SEQ_LEN, (chunk + 1) * SEQ_LEN)

    def weight(name, first, count):
        unit = UNIT[name]
        parts = []
        for tile in range(first, first + count):
            start = OFFSET[name] + unit * tile
            parts.append(slab[:, :, start : start + unit, :].reshape(NZ * NX * unit, LANES))
        return jnp.concatenate(parts, axis=1)

    def scaled(ref, chunk, gain, width):
        squares = jnp.zeros((SEQ_LEN, LANES), F32)
        for slot in range(TP):
            value = ref[slot, rows_of(chunk), :].astype(F32)
            wide[:, slot * width : (slot + 1) * width] = (
                value * gain[:, slot * width : (slot + 1) * width]
            ).astype(BF16)
            square = value * value
            for lane_tile in range(width // LANES):
                squares = squares + square[:, lane_tile * LANES : (lane_tile + 1) * LANES]
        mean = jnp.sum(squares, axis=1, keepdims=True) * (1.0 / (TP * width))
        return lax.rsqrt(mean + EPSILON)

    def product(lhs, name, first, count):
        return jnp.dot(lhs, weight(name, first, count), preferred_element_type=F32)

    def up_stage(source, gain, name, target):
        def run(chunk):
            factor = scaled(source, chunk, gain, 256)
            lhs = wide[...]
            p0 = product(lhs, name, 0, 2) * factor
            p1 = product(lhs, name, 2, 2) * factor
            p2 = product(lhs, name, 4, 2) * factor
            gates = (p0[:, :LANES], p0[:, LANES:], p1[:, :LANES])
            ups = (p1[:, LANES:], p2[:, :LANES], p2[:, LANES:])
            for tile in range(3):
                target[me, rows_of(chunk), tile * LANES : (tile + 1) * LANES] = (
                    silu(gates[tile]) * ups[tile]
                ).astype(BF16)
        return run

    def down_stage(source, name, residual, finish):
        def run(chunk):
            lhs = jnp.concatenate([source[slot, rows_of(chunk), :] for slot in range(TP)], axis=1)
            total = product(lhs, name, 0, 2)
            finish(chunk, (residual[me, rows_of(chunk), :].astype(F32) + 0.5 * total).astype(BF16))
        return run

    def finish_into(target):
        def finish(chunk, value):
            target[me, rows_of(chunk), :] = value
        return finish

    def finish_out(chunk, value):
        out[rows_of(chunk), :] = value

    def mix_stage(chunk):
        factor = scaled(x2, chunk, mix_gain, 256)
        both = product(wide[...], W3, 0, 2) * factor
        branch, gate_act = both[:, :LANES], both[:, LANES:]
        time = lax.broadcasted_iota(jnp.int32, (SEQ_LEN, LANES), 0)

        def earlier(value, k, fill):
            return jnp.where(time >= k, pltpu.roll(value, k, 0), fill)

        convolved = jnp.zeros((SEQ_LEN, LANES), F32)
        for k in range(4):
            lag = 3 - k
            shifted = branch if lag == 0 else earlier(branch, lag, 0.0)
            convolved = convolved + shifted * taps[k : k + 1, :]
        convolved = convolved.astype(BF16)
        retained = sigmoid(jnp.dot(convolved, blocks[0], preferred_element_type=F32))
        admitted = sigmoid(jnp.dot(convolved, blocks[1], preferred_element_type=F32))
        rate = DECAY_SCALE * softplus(-decay[...]) * retained
        add_now = jnp.sqrt(stable_one_minus_exp(2.0 * rate)) * admitted * convolved.astype(F32)
        keep = jnp.exp(-rate)
        k = 1
        while k < SEQ_LEN:
            add_now = keep * earlier(add_now, k, 0.0) + add_now
            if 2 * k < SEQ_LEN:
                keep = keep * earlier(keep, k, 1.0)
            k *= 2
        mixed[me, rows_of(chunk), :] = (add_now * gelu(gate_act)).astype(BF16)

    def out_stage(chunk):
        factor = scaled(mixed, chunk, channel_gain, 128)
        total = product(wide[:, : TP * LANES], W4, 0, 2) * factor
        x3[me, rows_of(chunk), :] = (x2[me, rows_of(chunk), :].astype(F32) + total).astype(BF16)

    stages = {
        1: (W1, up_stage(x1, pre_gain, W1, h1)),
        2: (W2, down_stage(h1, W2, x1, finish_into(x2))),
        3: (W3, mix_stage),
        4: (W4, out_stage),
        5: (W5, up_stage(x3, post_gain, W5, h2)),
        6: (W6, down_stage(h2, W6, x3, finish_out)),
    }

    def enter():
        token_load.wait()
        pl.semaphore_wait(barrier, len(neighbours))

    add(("build", "blocks"), build_blocks, cost=0.3, rank=3, after=(("compute", 1, 0),))
    add(("enter",), enter, after=(("build", W1),), rank=-5)
    for task in tasks:
        if task.name == ((0, "a1"), "start") or task.name == ((0, "b1"), "start"):
            task.after = task.after + (("enter",),)
        if task.name[0] == "build" and task.name[1] in (W2, W3, W4, W5, W6):
            task.after = task.after + (((0, "b1"), "start"), ((0, "a1"), "start"))
    for chunk in range(CHUNKS):
        add(("share", 1, chunk), functools.partial(share_own, 1, chunk),
            after=(("enter",),) if chunk == 0 else (("share", 1, chunk - 1),), sends=own_sends(1, chunk), rank=1)
    for stage in range(1, 7):
        for chunk in range(CHUNKS):
            share_tasks(stage, chunk)
            name, run = stages[stage]

            def compute(stage=stage, chunk=chunk, run=run):
                for n in range(4):
                    arrived((stage, chunk, ("d", n)))
                run(chunk)
                if stage < 6:
                    share_own(stage + 1, chunk)

            after = piece_done[PIECE_OF[name]] + (((stage, chunk), "third"),)
            if chunk:
                after = after + (("compute", stage, chunk - 1),)
            if stage == 3:
                after = after + (("build", "blocks"),)
            add(("compute", stage, chunk), compute, after=after, rank=2, cost=COST[stage],
                needs=tuple((stage, chunk, ("d", n)) for n in range(4)),
                sends=own_sends(stage + 1, chunk) if stage < 6 else [])

    for task in ordered(tasks):
        task.fn()
    for copy in copies.values():
        copy.wait_send()


def layer(
    tokens, pre_gain, pre_gate, pre_up, pre_down, mix_gain, branch_proj, gate_proj, conv_taps,
    retain_blocks, admit_blocks, decay_param, channel_gain, out_proj, post_gain, post_gate,
    post_up, post_down,
):
    large = (tokens, pre_gate, pre_up, pre_down, branch_proj, gate_proj, out_proj, post_gate, post_up, post_down)
    small = (
        pre_gain.reshape(1, -1), mix_gain.reshape(1, -1), channel_gain.reshape(1, -1),
        post_gain.reshape(1, -1), conv_taps, retain_blocks, admit_blocks, decay_param.reshape(1, -1),
    )
    return pl.pallas_call(
        kernel,
        out_shape=jax.ShapeDtypeStruct(tokens.shape, tokens.dtype),
        in_specs=[pl.BlockSpec(memory_space=pl.ANY)] * len(large)
        + [pl.BlockSpec(memory_space=pltpu.VMEM)] * len(small),
        out_specs=pl.BlockSpec(memory_space=pltpu.VMEM),
        scratch_shapes=[pltpu.VMEM(a.shape, F32) for a in large[1:]]
        + [
            pltpu.VMEM((NZ, NX, SLAB, LANES), BF16),
            pltpu.VMEM((TP, ROWS, 256), BF16),
            pltpu.VMEM((TP, ROWS, 256), BF16),
            pltpu.VMEM((TP, ROWS, 256), BF16),
            pltpu.VMEM((TP, ROWS, 384), BF16),
            pltpu.VMEM((TP, ROWS, 384), BF16),
            pltpu.VMEM((TP, ROWS, 128), BF16),
            pltpu.VMEM((SEQ_LEN, 2048), BF16),
            pltpu.VMEM((352, 384), BF16),
            pltpu.VMEM((2, LANES, LANES), BF16),
            pltpu.SemaphoreType.DMA((len(large),)),
            pltpu.SemaphoreType.DMA((MAX_COPIES,)),
            pltpu.SemaphoreType.DMA((MAX_COPIES,)),
        ],
        compiler_params=pltpu.CompilerParams(
            collective_id=0, has_side_effects=True, vmem_limit_bytes=56 * 1024 * 1024
        ),
        name="layer",
    )(*large, *small)


def solution(mesh):
    torus = Mesh(mesh.devices.reshape(NZ, NX, NY, 2), ("z", "x", "y", "c"))
    fs, tp = ("z", "x"), ("y", "c")
    split = P(fs, tp)
    placed = (
        split, P(), split, split, split, P(), split, split, P(None, tp), P(tp, None, None),
        P(tp, None, None), P(tp), P(), split, P(), split, split, split,
    )
    return jax.shard_map(layer, mesh=torus, in_specs=placed, out_specs=split, check_vma=False)
```

```python
import functools

import jax
import jax.numpy as jnp
from jax import lax
from jax.experimental import pallas as pl
from jax.experimental.pallas import tpu as pltpu
from jax.sharding import Mesh
from jax.sharding import PartitionSpec as P


EPSILON = 1e-06
DECAY_SCALE = 8.0
NZ, NX, NY = 8, 4, 4
TP = 8
SEQ_LEN = 128
ROWS = 512
CHUNKS = ROWS // SEQ_LEN
LANES = 128
BF16, F32 = jnp.bfloat16, jnp.float32
MESH = pl.DeviceIdType.MESH

W1, W2, W3, W4, W5, W6 = "W1", "W2", "W3", "W4", "W5", "W6"
UNIT = {W1: 64, W2: 96, W3: 64, W4: 32, W5: 64, W6: 96}
TILES = {W1: 6, W2: 2, W3: 2, W4: 2, W5: 6, W6: 2}
OFFSET = {}
SLAB = 0
for _name in (W1, W2, W3, W4, W5, W6):
    OFFSET[_name] = SLAB
    SLAB += UNIT[_name] * TILES[_name]

FINE_A, FINE_B = ((0,), (1,), (2,)), ((0,), (1,), (2,), (3,), (4,))
COARSE_A, COARSE_B = ((0, 1, 2),), ((0, 1), (2, 3, 4))
PIECES = (
    ("1a", OFFSET[W1], 48, 80, (W1,), FINE_A, FINE_B),
    ("1b", OFFSET[W1] + 128, 48, 80, (W1,), FINE_A, FINE_B),
    ("1c", OFFSET[W1] + 256, 48, 80, (W1,), FINE_A, FINE_B),
    ("2", OFFSET[W2], 80, 112, (W2,), COARSE_A, COARSE_B),
    ("34", OFFSET[W3], 80, 112, (W3, W4), COARSE_A, COARSE_B),
    ("5", OFFSET[W5], 160, 224, (W5,), COARSE_A, COARSE_B),
    ("6", OFFSET[W6], 80, 112, (W6,), COARSE_A, COARSE_B),
)

HALVES, QUARTERS = ((0, 256), (256, 256)), tuple((n * SEQ_LEN, SEQ_LEN) for n in range(CHUNKS))
UNITS = {
    1: tuple((r, n, 0, 256) for r, n in QUARTERS),
    2: tuple((r, n, t * 128, 128) for t in range(2) for r, n in HALVES) + tuple((r, n, 256, 128) for r, n in QUARTERS),
    3: tuple((r, n, 0, 256) for r, n in QUARTERS),
    4: tuple((r, n, 0, 128) for r, n in QUARTERS),
    5: tuple((r, n, 0, 256) for r, n in QUARTERS),
    6: tuple((r, n, 0, 384) for r, n in QUARTERS),
}

SEMS = 320
LINK_RATE, CHIP_RATE = 91e3, 500e3
LINK_LATENCY, CHIP_LATENCY = 1.8, 1.0
BACKLOG = 60e3
COST = {"norm": 0.25, "tile": 0.2, 2: 0.55, 3: 0.8, 4: 0.3, 6: 0.55}


class Task:
    def __init__(self, name, fn, after=(), needs=(), sends=(), cost=0.05, rank=0, gate=None):
        self.name, self.fn, self.after, self.needs = name, fn, tuple(after), tuple(needs)
        self.sends, self.cost, self.rank, self.gate = tuple(sends), cost, rank, gate


class Links:
    def __init__(self):
        self.now, self.queues, self.arrival = 0.0, {}, {}

    def flows(self):
        found = []
        for axis in "xyz":
            heads = [q for q in (axis + "f", axis + "b") if self.queues.get(q)]
            found += [(q, LINK_RATE / len(heads), LINK_LATENCY) for q in heads]
        if self.queues.get("d"):
            found.append(("d", CHIP_RATE, CHIP_LATENCY))
        return found

    def advance(self, until):
        while True:
            flows = self.flows()
            step = min([self.queues[q][0][1] / rate for q, rate, _ in flows], default=1e9)
            if self.now + step > until:
                for q, rate, _ in flows:
                    self.queues[q][0][1] -= rate * (until - self.now)
                self.now = until
                return
            self.now += step
            for q, rate, latency in flows:
                head = self.queues[q][0]
                head[1] -= rate * step
                if head[1] <= 1e-3:
                    self.queues[q].pop(0)
                    self.arrival[head[0]] = self.now + latency

    def next_event(self):
        times = [t for t in self.arrival.values() if t > self.now + 1e-9]
        times += [self.now + self.queues[q][0][1] / rate + 1e-6 for q, rate, _ in self.flows()]
        return min(times)

    def backlog(self, axis):
        return sum(size for q in (axis + "f", axis + "b") for _, size in self.queues.get(q, ()))


def ordered(tasks):
    links, done, order, left = Links(), set(), [], list(tasks)
    waiting = {}
    trace = []
    while left:
        best = None
        for task in left:
            if not all(a in done for a in task.after):
                continue
            ready = 0.0
            for m in task.needs:
                ready = max(ready, links.arrival.get(m, 1e9))
            if ready > links.now or (task.gate and links.backlog(task.gate) > BACKLOG):
                continue
            if best is None or (task.rank, ready) < best[0]:
                best = ((task.rank, ready), task)
        if best is None:
            links.advance(links.next_event())
            continue
        task = best[1]
        trace.append((links.now, task.name))
        links.advance(links.now + task.cost)
        for message, queue, size in task.sends:
            links.queues.setdefault(queue, []).append([message, size])
        done.add(task.name)
        left.remove(task)
        order.append(task)
    ordered.trace, ordered.end = trace, links.now
    return order


def stable_one_minus_exp(t):
    series = 1.0 - t * (1.0 / 8.0)
    for n in (7.0, 6.0, 5.0, 4.0, 3.0, 2.0):
        series = 1.0 - t * (1.0 / n) * series
    return jnp.where(t < 0.5, t * series, 1.0 - jnp.exp(-t))


def softplus(v):
    e = jnp.exp(-jnp.abs(v))
    u = e / (2.0 + e)
    s = u * u
    total = jnp.zeros_like(s)
    for n in (19, 17, 15, 13, 11, 9, 7, 5, 3, 1):
        total = total * s + 1.0 / n
    return jnp.maximum(v, 0.0) + 2.0 * u * total


def silu(v):
    return v / (1.0 + jnp.exp(-v))


def sigmoid(v):
    return 1.0 / (1.0 + jnp.exp(-v))


def gelu(v):
    return 0.5 * v * (1.0 + jnp.tanh(0.7978845608028654 * (v + 0.044715 * (v * v * v))))


def kernel(
    tokens, pre_gate, pre_up, pre_down, branch_proj, gate_proj, out_proj, post_gate, post_up,
    post_down, pre_gain, mix_gain, channel_gain, post_gain, taps, retain, admit, decay,
    out,
    s_pre_gate, s_pre_up, s_pre_down, s_branch, s_gate, s_out, s_post_gate, s_post_up, s_post_down,
    slab, x1, x2, x3, h1, h2, mixed, wide, factors, spread, blocks, local_sem, sems,
):
    z, x, y, c = (lax.axis_index(a) for a in ("z", "x", "y", "c"))
    step = 1 - 2 * c
    me = y * 2 + c

    shards = {
        "pre_gate": (pre_gate, s_pre_gate), "pre_up": (pre_up, s_pre_up),
        "pre_down": (pre_down, s_pre_down), "branch": (branch_proj, s_branch),
        "gate": (gate_proj, s_gate), "out": (out_proj, s_out),
        "post_gate": (post_gate, s_post_gate), "post_up": (post_up, s_post_up),
        "post_down": (post_down, s_post_down),
    }
    loads = {}
    for n, (key, (src, dst)) in enumerate(shards.items()):
        loads[key] = pltpu.make_async_copy(src, dst, local_sem.at[n])
        loads[key].start()
    token_load = pltpu.make_async_copy(tokens, x1.at[me], local_sem.at[len(shards)])
    token_load.start()

    def toward(axis, n, index, distance):
        return {axis: lax.rem(index + distance + n, n)}

    neighbours = [toward(a, n, i, d) for a, n, i in (("z", NZ, z), ("x", NX, x), ("y", NY, y)) for d in (1, -1)]
    neighbours.append({"c": 1 - c})
    barrier = pltpu.get_barrier_semaphore()
    for device in neighbours:
        pl.semaphore_signal(barrier, inc=1, device_id=device, device_id_type=MESH)

    used = {"recv": 0}
    recv_of, drains = {}, []

    def take():
        used["recv"] += 1
        return sems.at[used["recv"] - 1]

    def receipt(message):
        if message not in recv_of:
            recv_of[message] = take()
        return recv_of[message]

    def send(message, send_sem, ref, device):
        pltpu.make_async_remote_copy(
            src_ref=ref, dst_ref=ref, send_sem=send_sem, recv_sem=receipt(message),
            device_id=device, device_id_type=MESH,
        ).start()

    def await_bytes(ref, sem):
        pltpu.make_async_copy(ref, ref, sem).wait()

    lane = lax.broadcasted_iota(jnp.int32, (352, 384), 1)
    row = lax.broadcasted_iota(jnp.int32, (352, 384), 0)
    group = (lane >= 96).astype(jnp.int32) + (lane >= 192).astype(jnp.int32) + (lane >= 288).astype(jnp.int32)
    spread[...] = jnp.where((row == lane - 8 * group) & (lane - 96 * group < 88), 1.0, 0.0).astype(BF16)

    def put(name, tile, value):
        start = OFFSET[name] + UNIT[name] * tile
        slab[z, x, start : start + UNIT[name], :] = value.astype(BF16)

    def build_wide(name, gate_key, up_key):
        for half, key in enumerate((gate_key, up_key)):
            loads[key].wait()
            placed = jnp.dot(shards[key][1][...].astype(BF16), spread[...], preferred_element_type=F32)
            for tile in range(3):
                put(name, half + 2 * tile, placed[:, tile * LANES : (tile + 1) * LANES])

    def build_down(name, key):
        loads[key].wait()
        for tile in range(2):
            value = shards[key][1][:, tile * LANES : (tile + 1) * LANES]
            put(name, tile, jnp.concatenate((value, jnp.zeros((8, LANES), F32)), axis=0))

    def build_mixer():
        loads["branch"].wait()
        put(W3, 0, s_branch[...])
        loads["gate"].wait()
        put(W3, 1, s_gate[...])

    def build_out():
        loads["out"].wait()
        for tile in range(2):
            put(W4, tile, s_out[:, tile * LANES : (tile + 1) * LANES])

    def build_blocks():
        tall = lax.broadcasted_iota(jnp.int32, (LANES, 64), 0)
        flat = lax.broadcasted_iota(jnp.int32, (LANES, 64), 1)
        wide_r = lax.broadcasted_iota(jnp.int32, (64, LANES), 0)
        wide_c = lax.broadcasted_iota(jnp.int32, (64, LANES), 1)
        for n, ref in enumerate((retain, admit)):
            total = jnp.zeros((LANES, LANES), F32)
            for b in range(2):
                left = jnp.where(tall == flat + 64 * b, 1.0, 0.0).astype(BF16)
                right = jnp.where(wide_c == wide_r + 64 * b, 1.0, 0.0).astype(BF16)
                spread_b = jnp.dot(ref[b].astype(BF16), right, preferred_element_type=F32).astype(BF16)
                total = total + jnp.dot(left, spread_b, preferred_element_type=F32)
            blocks[n] = total.astype(BF16)

    builds = {
        W1: lambda: build_wide(W1, "pre_gate", "pre_up"),
        W2: lambda: build_down(W2, "pre_down"),
        W3: build_mixer,
        W4: build_out,
        W5: lambda: build_wide(W5, "post_gate", "post_up"),
        W6: lambda: build_down(W6, "post_down"),
    }

    tasks = []

    def add(*args, **kwargs):
        tasks.append(Task(*args, **kwargs))

    def ring(label, axis, groups, block, blocks_of, rank, size):
        n, index = {"x": (NX, x), "z": (NZ, z)}[axis]
        far = n // 2
        send_sem = take()
        total = n - 1
        count = sum(len(group) for group in groups)
        drains.append((blocks_of(total, count), send_sem))
        starts = []
        for g, group in enumerate(groups):
            width = len(group)

            def hop(way, k, group=group, g=g):
                sign = step if way == "f" else -step
                origin = lax.rem(index - sign * (k - 1) + n, n)
                for member in group:
                    ref = block(origin, member)
                    send((label, g, k), send_sem, ref, toward(axis, n, index, sign))

            def queued(k, g=g, width=width):
                ways = "fb" if k < far else "f"
                return [((label, g, k, way), axis + way, size * width) for way in ways]

            names = []
            for k in range(1, far + 1):
                def relay(k=k, hop=hop, g=g, width=width):
                    await_bytes(blocks_of(2 if k < far else 1, width), recv_of[(label, g, k)])
                    if k < far:
                        hop("f", k + 1)
                    if k < far - 1:
                        hop("b", k + 1)
                names.append((label, g, k))
                needs = [m for m, _, _ in queued(k)]
                starts_k = relay
                ring_tasks[(label, g, k)] = Task(
                    (label, g, k), relay, after=((label, g, k - 1),), needs=needs, rank=rank,
                    sends=queued(k + 1) if k < far else (), cost=0.07)

            def begin(hop=hop):
                hop("f", 1)
                hop("b", 1)

            starts.append((begin, queued(1), names))
        return starts

    ring_tasks = {}
    piece_done = {}
    for p, (label, first, rows_a, rows_b, needed, groups_a, groups_b) in enumerate(PIECES):
        for name in needed:
            if not any(task.name == ("build", name) for task in tasks):
                add(("build", name), builds[name], cost=0.4 if name == W5 else 0.1, rank=p)
        span_a, span_b = slice(first, first + rows_a), slice(first + rows_a, first + rows_a + rows_b)
        size_a, size_b = rows_a * LANES * 2, rows_b * LANES * 2

        def bytes_a(ways, width, s=span_a):
            return slab.at[pl.ds(0, ways), pl.ds(0, width), s, :]

        def bytes_b(ways, width, s=span_b):
            return slab.at[pl.ds(0, width), pl.ds(0, ways), s, :]

        def first_ring(part, axis, block, size, blocks_of, second, groups):
            n = {"x": NX, "z": NZ}[axis]
            far = n // 2
            [(begin, queued, names)] = ring((label, part, axis), axis, ((None,),), block, blocks_of, p, size)
            key = (label, part, axis, "start")
            ready = tuple(("build", name) for name in needed) + (("enter",),)
            starters = {}
            for g, group in enumerate(groups):
                starters.setdefault(group[-1], []).append(g)

            def launch(k):
                for g in starters.get(k, ()):
                    second[g][0]()

            def launch_sends(k):
                return [m for g in starters.get(k, ()) for m in second[g][1]]

            def starting():
                begin()
                launch(0)

            add(key, starting, after=ready, rank=p, sends=list(queued) + launch_sends(0), cost=0.1, gate=axis)
            previous, last = key, None
            for k, name in enumerate(names, 1):
                task = ring_tasks[name]

                def run(inner=task.fn, k=k):
                    inner()
                    launch(k)

                add(name, run, after=(previous,), needs=task.needs, rank=p, cost=0.1,
                    sends=task.sends + tuple(launch_sends(k)))
                previous = name
            ends = []
            for g, group in enumerate(groups):
                begun = key if group[-1] == 0 else names[group[-1] - 1]
                for k, name in enumerate(second[g][2], 1):
                    task = ring_tasks[name]
                    add(name, task.fn, after=(begun if k == 1 else second[g][2][k - 2],), needs=task.needs,
                        rank=p, sends=task.sends, cost=0.07)
                ends.append(second[g][2][-1])
            return (previous,) + tuple(ends)

        def members_a(group):
            return tuple(d for k in group for d in ((0,) if k == 0 else (-step, step) if k == 1 else (2,)))

        def members_b(group):
            return tuple(d for k in group for d in ((0,) if k == 0 else (-step * k, step * k) if k < 4 else (4,)))

        second_a = ring(
            (label, "a", "z"), "z", tuple(members_a(g) for g in groups_a),
            lambda i, d, s=span_a: slab.at[i, lax.rem(x + d + NX, NX), s, :], bytes_a, p, size_a)
        second_b = ring(
            (label, "b", "x"), "x", tuple(members_b(g) for g in groups_b),
            lambda i, d, s=span_b: slab.at[lax.rem(z + d + NZ, NZ), i, s, :], bytes_b, p, size_b)
        done_a = first_ring(
            "a", "x", lambda i, _, s=span_a: slab.at[z, i, s, :], size_a, bytes_a, second_a, groups_a)
        done_b = first_ring(
            "b", "z", lambda i, _, s=span_b: slab.at[i, x, s, :], size_b,
            lambda ways, width, s=span_b: slab.at[pl.ds(0, ways), pl.ds(0, width), s, :], second_b, groups_b)
        piece_done[label] = done_a + done_b
        if p:
            for task in tasks:
                if task.name in ((label, "a", "x", "start"), (label, "b", "z", "start")):
                    task.after = task.after + ((PIECES[p - 1][0],) + task.name[1:],)

    held = {1: x1, 2: h1, 3: x2, 4: mixed, 5: x3, 6: h2}
    share_sems = {stage: take() for stage in held}
    for stage, ref in held.items():
        drains.append((ref.at[pl.ds(0, 7)], share_sems[stage]))
    up, down, partner = toward("y", NY, y, step), toward("y", NY, y, -step), {"c": 1 - c}

    def slot_at(distance):
        return lax.rem(y + distance + NY, NY) * 2 + c

    def part_of(stage, unit, slots):
        row, rows, first, lanes = UNITS[stage][unit]
        return held[stage].at[slots, row : row + rows, first : first + lanes]

    def share(stage, unit, slot, hops):
        for tag, device in hops:
            send((stage, unit, tag), share_sems[stage], part_of(stage, unit, slot), device)

    def share_own(stage, unit):
        share(stage, unit, me, (("near", up), ("near", down), ("d", partner)))

    def unit_size(stage, unit):
        return UNITS[stage][unit][1] * UNITS[stage][unit][3] * 2

    def own_sends(stage, unit):
        size = unit_size(stage, unit)
        return [((stage, unit, "f1"), "yf", size), ((stage, unit, "b1"), "yb", size), ((stage, unit, "d0"), "d", size)]

    def share_tasks(stage, unit):
        size = unit_size(stage, unit)

        def first():
            await_bytes(part_of(stage, unit, pl.ds(0, 2)), recv_of[(stage, unit, "near")])
            share(stage, unit, slot_at(-step), (("far", up), ("d", partner)))
            share(stage, unit, slot_at(step), (("d", partner),))

        def second():
            await_bytes(part_of(stage, unit, 0), recv_of[(stage, unit, "far")])
            share(stage, unit, slot_at(2), (("d", partner),))

        add((stage, unit, "first"), first, needs=((stage, unit, "f1"), (stage, unit, "b1")), rank=-2, cost=0.1,
            sends=[((stage, unit, "f2"), "yf", size), ((stage, unit, "d1"), "d", size), ((stage, unit, "d2"), "d", size)])
        add((stage, unit, "second"), second, after=((stage, unit, "first"),), needs=((stage, unit, "f2"),), rank=-2,
            sends=[((stage, unit, "d3"), "d", size)])

    def rows_of(chunk):
        return slice(chunk * SEQ_LEN, (chunk + 1) * SEQ_LEN)

    def weight(name, first, count):
        unit = UNIT[name]
        parts = []
        for tile in range(first, first + count):
            start = OFFSET[name] + unit * tile
            parts.append(slab[:, :, start : start + unit, :].reshape(NZ * NX * unit, LANES))
        return jnp.concatenate(parts, axis=1)

    def normalized(ref, chunk, gain, width):
        squares = jnp.zeros((SEQ_LEN, LANES), F32)
        for slot in range(TP):
            value = ref[slot, rows_of(chunk), :].astype(F32)
            wide[rows_of(chunk), slot * width : (slot + 1) * width] = (
                value * gain[:, slot * width : (slot + 1) * width]
            ).astype(BF16)
            square = value * value
            for lane_tile in range(width // LANES):
                squares = squares + square[:, lane_tile * LANES : (lane_tile + 1) * LANES]
        mean = jnp.sum(squares, axis=1, keepdims=True) * (1.0 / (TP * width))
        factor = jnp.broadcast_to(lax.rsqrt(mean + EPSILON), (SEQ_LEN, LANES))
        factors[rows_of(chunk), :] = factor
        return factor

    def product(lhs, name, first, count):
        return jnp.dot(lhs, weight(name, first, count), preferred_element_type=F32)

    def up_unit(name, target, unit):
        row, rows, first, lanes = unit
        span = slice(row, row + rows)
        factor = factors[span, :]
        for tile in range(first // LANES, (first + lanes) // LANES):
            both = product(wide[span, :], name, 2 * tile, 2)
            target[me, span, tile * LANES : (tile + 1) * LANES] = (
                silu(both[:, :LANES] * factor) * (both[:, LANES:] * factor)
            ).astype(BF16)

    def down_stage(source, name, residual, finish):
        def run(chunk):
            lhs = jnp.concatenate([source[slot, rows_of(chunk), :] for slot in range(TP)], axis=1)
            total = product(lhs, name, 0, 2)
            finish(chunk, (residual[me, rows_of(chunk), :].astype(F32) + 0.5 * total).astype(BF16))
        return run

    def finish_into(target):
        def finish(chunk, value):
            target[me, rows_of(chunk), :] = value
        return finish

    def finish_out(chunk, value):
        out[rows_of(chunk), :] = value

    def mix_stage(chunk):
        factor = normalized(x2, chunk, mix_gain, 256)
        both = product(wide[rows_of(chunk), :], W3, 0, 2)
        branch, gate_act = both[:, :LANES] * factor, both[:, LANES:] * factor
        time = lax.broadcasted_iota(jnp.int32, (SEQ_LEN, LANES), 0)

        def earlier(value, k, fill):
            return jnp.where(time >= k, pltpu.roll(value, k, 0), fill)

        convolved = jnp.zeros((SEQ_LEN, LANES), F32)
        for k in range(4):
            lag = 3 - k
            shifted = branch if lag == 0 else earlier(branch, lag, 0.0)
            convolved = convolved + shifted * taps[k : k + 1, :]
        convolved = convolved.astype(BF16)
        retained = sigmoid(jnp.dot(convolved, blocks[0], preferred_element_type=F32))
        admitted = sigmoid(jnp.dot(convolved, blocks[1], preferred_element_type=F32))
        rate = DECAY_SCALE * softplus(-decay[...]) * retained
        add_now = jnp.sqrt(stable_one_minus_exp(2.0 * rate)) * admitted * convolved.astype(F32)
        keep = jnp.exp(-rate)
        k = 1
        while k < SEQ_LEN:
            add_now = keep * earlier(add_now, k, 0.0) + add_now
            if 2 * k < SEQ_LEN:
                keep = keep * earlier(keep, k, 1.0)
            k *= 2
        mixed[me, rows_of(chunk), :] = (add_now * gelu(gate_act)).astype(BF16)

    def out_stage(chunk):
        factor = normalized(mixed, chunk, channel_gain, 128)
        total = product(wide[rows_of(chunk), : TP * LANES], W4, 0, 2) * jnp.concatenate((factor, factor), axis=1)
        x3[me, rows_of(chunk), :] = (x2[me, rows_of(chunk), :].astype(F32) + total).astype(BF16)

    def enter():
        token_load.wait()
        pl.semaphore_wait(barrier, len(neighbours))

    add(("enter",), enter, after=(("build", W1),), rank=-5)
    add(("build", "blocks"), build_blocks, cost=0.3, rank=3, after=(("enter",),))
    first_sends = ((PIECES[0][0], "a", "x", "start"), (PIECES[0][0], "b", "z", "start"))
    for task in tasks:
        if task.name[0] == "build" and task.name[1] != W1:
            task.after = task.after + first_sends
    for unit in range(len(UNITS[1])):
        add(("share", 1, unit), functools.partial(share_own, 1, unit), after=first_sends, sends=own_sends(1, unit), rank=1)
    for stage in held:
        for unit in range(len(UNITS[stage])):
            share_tasks(stage, unit)

    def inputs(stage, chunk):
        row = chunk * SEQ_LEN
        units = [u for u, (r, n, _, _) in enumerate(UNITS[stage]) if r <= row < r + n]
        return units, [(stage, u, "d%d" % n) for u in units for n in range(4)], [(stage, u, "second") for u in units]

    received = set()

    def receive(stage, chunk):
        for unit in inputs(stage, chunk)[0]:
            if (stage, unit) not in received:
                received.add((stage, unit))
                await_bytes(part_of(stage, unit, pl.ds(0, 4)), recv_of[(stage, unit, "d")])

    def add_up(stage, source, gain, name, target, labels):
        for chunk in range(CHUNKS):
            def norm(chunk=chunk):
                receive(stage, chunk)
                normalized(source, chunk, gain, 256)
            _, needs, after = inputs(stage, chunk)
            if stage == 5:
                after = after + [("compute", 4, n) for n in range(CHUNKS)]
            add(("norm", stage, chunk), norm, after=after, needs=needs, cost=COST["norm"], rank=2)
        for u, unit in enumerate(UNITS[stage + 1]):
            row, rows, first, lanes = unit
            def run(u=u, unit=unit):
                up_unit(name, target, unit)
                share_own(stage + 1, u)
            pieces = labels[first // LANES : (first + lanes) // LANES]
            after = [t for piece in pieces for t in piece_done[piece]]
            after += [("norm", stage, n) for n in range(row // SEQ_LEN, (row + rows) // SEQ_LEN)]
            add(("tile", stage, u), run, after=after, sends=own_sends(stage + 1, u), rank=-1,
                cost=COST["tile"] * rows * lanes / (SEQ_LEN * LANES))

    def add_rows(stage, run, piece, before=()):
        for chunk in range(CHUNKS):
            def compute(chunk=chunk):
                receive(stage, chunk)
                run(chunk)
                if stage < 6:
                    share_own(stage + 1, chunk)
            _, needs, after = inputs(stage, chunk)
            after = after + list(piece_done[piece]) + list(before(chunk) if before else ())
            add(("compute", stage, chunk), compute, after=after, needs=needs, rank=-1, cost=COST[stage],
                sends=own_sends(stage + 1, chunk) if stage < 6 else ())

    add_up(1, x1, pre_gain, W1, h1, ("1a", "1b", "1c"))
    add_rows(2, down_stage(h1, W2, x1, finish_into(x2)), "2")
    add_rows(3, mix_stage, "34", lambda chunk: [("build", "blocks")] + [("tile", 1, u) for u in range(len(UNITS[2]))])
    add_rows(4, out_stage, "34")
    add_up(5, x3, post_gain, W5, h2, ("5", "5", "5"))
    add_rows(6, down_stage(h2, W6, x3, finish_out), "6")

    for task in ordered(tasks):
        task.fn()
    for ref, sem in drains:
        await_bytes(ref, sem)
    assert used["recv"] <= SEMS, used["recv"]


def layer(
    tokens, pre_gain, pre_gate, pre_up, pre_down, mix_gain, branch_proj, gate_proj, conv_taps,
    retain_blocks, admit_blocks, decay_param, channel_gain, out_proj, post_gain, post_gate,
    post_up, post_down,
):
    large = (tokens, pre_gate, pre_up, pre_down, branch_proj, gate_proj, out_proj, post_gate, post_up, post_down)
    small = (
        pre_gain.reshape(1, -1), mix_gain.reshape(1, -1), channel_gain.reshape(1, -1),
        post_gain.reshape(1, -1), conv_taps, retain_blocks, admit_blocks, decay_param.reshape(1, -1),
    )
    return pl.pallas_call(
        kernel,
        out_shape=jax.ShapeDtypeStruct(tokens.shape, tokens.dtype),
        in_specs=[pl.BlockSpec(memory_space=pl.ANY)] * len(large)
        + [pl.BlockSpec(memory_space=pltpu.VMEM)] * len(small),
        out_specs=pl.BlockSpec(memory_space=pltpu.VMEM),
        scratch_shapes=[pltpu.VMEM(a.shape, F32) for a in large[1:]]
        + [
            pltpu.VMEM((NZ, NX, SLAB, LANES), BF16),
            pltpu.VMEM((TP, ROWS, 256), BF16),
            pltpu.VMEM((TP, ROWS, 256), BF16),
            pltpu.VMEM((TP, ROWS, 256), BF16),
            pltpu.VMEM((TP, ROWS, 384), BF16),
            pltpu.VMEM((TP, ROWS, 384), BF16),
            pltpu.VMEM((TP, ROWS, 128), BF16),
            pltpu.VMEM((ROWS, 2048), BF16),
            pltpu.VMEM((ROWS, LANES), F32),
            pltpu.VMEM((352, 384), BF16),
            pltpu.VMEM((2, LANES, LANES), BF16),
            pltpu.SemaphoreType.DMA((len(large),)),
            pltpu.SemaphoreType.DMA((SEMS,)),
        ],
        compiler_params=pltpu.CompilerParams(
            collective_id=0, has_side_effects=True, vmem_limit_bytes=56 * 1024 * 1024
        ),
        name="layer",
    )(*large, *small)


def solution(mesh):
    torus = Mesh(mesh.devices.reshape(NZ, NX, NY, 2), ("z", "x", "y", "c"))
    fs, tp = ("z", "x"), ("y", "c")
    split = P(fs, tp)
    placed = (
        split, P(), split, split, split, P(), split, split, P(None, tp), P(tp, None, None),
        P(tp, None, None), P(tp), P(), split, P(), split, split, split,
    )
    return jax.shard_map(layer, mesh=torus, in_specs=placed, out_specs=split, check_vma=False)
```

```python
import functools

import jax
import jax.numpy as jnp
from jax import lax
from jax.experimental import pallas as pl
from jax.experimental.pallas import tpu as pltpu
from jax.sharding import Mesh
from jax.sharding import PartitionSpec as P


EPSILON = 1e-06
DECAY_SCALE = 8.0
NZ, NX, NY = 8, 4, 4
TP = 8
SEQ_LEN = 128
ROWS = 512
CHUNKS = ROWS // SEQ_LEN
LANES = 128
BF16, F32 = jnp.bfloat16, jnp.float32
MESH = pl.DeviceIdType.MESH

W1, W2, W3, W4, W5, W6 = "W1", "W2", "W3", "W4", "W5", "W6"
UNIT = {W1: 64, W2: 96, W3: 64, W4: 32, W5: 64, W6: 96}
TILES = {W1: 6, W2: 2, W3: 2, W4: 2, W5: 6, W6: 2}
OFFSET = {}
SLAB = 0
for _name in (W1, W2, W3, W4, W5, W6):
    OFFSET[_name] = SLAB
    SLAB += UNIT[_name] * TILES[_name]

FINE_A, FINE_B = ((0,), (1,), (2,)), ((0,), (1,), (2,), (3,), (4,))
COARSE_A, COARSE_B = ((0, 1, 2),), ((0, 1), (2, 3, 4))
PIECES = (
    ("1a", OFFSET[W1], 48, 80, (W1,), FINE_A, FINE_B),
    ("1b", OFFSET[W1] + 128, 48, 80, (W1,), FINE_A, FINE_B),
    ("1c", OFFSET[W1] + 256, 48, 80, (W1,), FINE_A, FINE_B),
    ("2", OFFSET[W2], 80, 112, (W2,), COARSE_A, COARSE_B),
    ("34", OFFSET[W3], 80, 112, (W3, W4), COARSE_A, COARSE_B),
    ("5", OFFSET[W5], 160, 224, (W5,), COARSE_A, COARSE_B),
    ("6", OFFSET[W6], 80, 112, (W6,), COARSE_A, COARSE_B),
)

HALVES, QUARTERS = ((0, 256), (256, 256)), tuple((n * SEQ_LEN, SEQ_LEN) for n in range(CHUNKS))
UNITS = {
    1: tuple((r, n, 0, 256) for r, n in QUARTERS),
    2: tuple((r, n, t * 128, 128) for t in range(2) for r, n in HALVES) + tuple((r, n, 256, 128) for r, n in QUARTERS),
    3: tuple((r, n, 0, 256) for r, n in QUARTERS),
    4: tuple((r, n, 0, 128) for r, n in QUARTERS),
    5: tuple((r, n, 0, 256) for r, n in QUARTERS),
    6: tuple((r, n, 0, 384) for r, n in QUARTERS),
}

SEMS = 258
LINK_RATE, CHIP_RATE = 91e3, 500e3
LINK_LATENCY, CHIP_LATENCY = 3.00, 1.0
HOLD, MARGIN = 100000, 0
GATES = {
    "a1a": ("z", 1000000),
    "a1b": ("z", 1000000),
    "a1c": ("z", 4000000),
    "a2": ("z", 1000000),
    "a34": ("z", 500000),
    "a5": ("z", 1000000),
    "a6": ("x", 356000),
    "b1a": ("z", 500000),
    "b1b": ("z", 700000),
    "b1c": ("z", 3400000),
    "b2": ("x", 1200000),
    "b34": ("z", 866000),
    "b5": ("x", 1000000),
    "b6": ("z", 364000),
}
COST = {"norm": 0.23, "tile": 0.2, 2: 0.57, 3: 0.8, 4: 0.3, 6: 0.55}


class Task:
    def __init__(self, name, fn, after=(), needs=(), sends=(), cost=0.05, rank=0, gate=None, held=False):
        self.name, self.fn, self.after, self.needs = name, fn, tuple(after), tuple(needs)
        self.sends, self.cost, self.rank, self.gate, self.held = tuple(sends), cost, rank, gate, held


class Links:
    def __init__(self):
        self.now, self.queues, self.arrival = 0.0, {}, {}

    def flows(self):
        found = []
        for axis in "xyz":
            heads = [q for q in (axis + "f", axis + "b") if self.queues.get(q)]
            found += [(q, LINK_RATE / len(heads), LINK_LATENCY) for q in heads]
        if self.queues.get("d"):
            found.append(("d", CHIP_RATE, CHIP_LATENCY))
        return found

    def advance(self, until):
        while True:
            flows = self.flows()
            step = min([self.queues[q][0][1] / rate for q, rate, _ in flows], default=1e9)
            if self.now + step > until:
                for q, rate, _ in flows:
                    self.queues[q][0][1] -= rate * (until - self.now)
                self.now = until
                return
            self.now += step
            for q, rate, latency in flows:
                head = self.queues[q][0]
                head[1] -= rate * step
                if head[1] <= 1e-3:
                    self.queues[q].pop(0)
                    self.arrival[head[0]] = self.now + latency

    def backlog(self, axis):
        return sum(size for q in (axis + "f", axis + "b") for _, size in self.queues.get(q, ()))

    def next_event(self):
        times = [t + m for t in self.arrival.values() for m in (0.0, MARGIN) if t + m > self.now + 1e-9]
        times += [self.now + self.queues[q][0][1] / rate + 1e-6 for q, rate, _ in self.flows()]
        return min(times)


def ordered(tasks):
    links, done, order, left = Links(), set(), [], list(tasks)
    trace = []
    pieces = [piece[0] for piece in PIECES]
    work = {}
    for task in tasks:
        for message, queue, size in task.sends:
            work[message] = (message[0][0] if isinstance(message[0], tuple) else None, queue[0], size)

    def shut(gate):
        axis, label, limit = gate
        earlier = pieces[: pieces.index(label)]
        rest = sum(
            size for m, (piece, a, size) in work.items() if a == axis and piece in earlier and m not in links.arrival)
        return rest > limit

    while left:
        best = None
        lead = min((task.rank for task in left if task.held), default=0)
        for task in left:
            if not all(a in done for a in task.after):
                continue
            if task.held and task.rank > lead and any(links.backlog(q[0]) > HOLD for _, q, _ in task.sends):
                continue
            ready = 0.0
            for m in task.needs:
                ready = max(ready, links.arrival.get(m, 1e9))
            if task.held and task.needs and task.rank > 2:
                ready += MARGIN
            if ready > links.now or (task.gate and shut(task.gate)):
                continue
            if best is None or (task.rank, ready) < best[0]:
                best = ((task.rank, ready), task)
        if best is None:
            links.advance(links.next_event())
            continue
        task = best[1]
        trace.append((links.now, task.name))
        links.advance(links.now + task.cost)
        for message, queue, size in task.sends:
            links.queues.setdefault(queue, []).append([message, size])
        done.add(task.name)
        left.remove(task)
        order.append(task)
    ordered.trace, ordered.end = trace, links.now
    return order


def stable_one_minus_exp(t):
    series = 1.0 - t * (1.0 / 8.0)
    for n in (7.0, 6.0, 5.0, 4.0, 3.0, 2.0):
        series = 1.0 - t * (1.0 / n) * series
    return jnp.where(t < 0.5, t * series, 1.0 - jnp.exp(-t))


def softplus(v):
    e = jnp.exp(-jnp.abs(v))
    u = e / (2.0 + e)
    s = u * u
    total = jnp.zeros_like(s)
    for n in (19, 17, 15, 13, 11, 9, 7, 5, 3, 1):
        total = total * s + 1.0 / n
    return jnp.maximum(v, 0.0) + 2.0 * u * total


def silu(v):
    return v / (1.0 + jnp.exp(-v))


def sigmoid(v):
    return 1.0 / (1.0 + jnp.exp(-v))


def gelu(v):
    return 0.5 * v * (1.0 + jnp.tanh(0.7978845608028654 * (v + 0.044715 * (v * v * v))))


def kernel(
    tokens, pre_gate, pre_up, pre_down, branch_proj, gate_proj, out_proj, post_gate, post_up,
    post_down, h_pre_gain, h_mix_gain, h_channel_gain, h_post_gain, h_taps, h_retain, h_admit, h_decay,
    out,
    s_pre_gate, s_pre_up, s_pre_down, s_branch, s_gate, s_out, s_post_gate, s_post_up, s_post_down,
    pre_gain, mix_gain, channel_gain, post_gain, taps, retain, admit, decay, result,
    slab, x1, x2, x3, h1, h2, mixed, wide, factors, spread, blocks, local_sem, sems,
):
    z, x, y, c = (lax.axis_index(a) for a in ("z", "x", "y", "c"))
    step = 1 - 2 * c
    me = y * 2 + c

    shards = {
        "pre_gate": (pre_gate, s_pre_gate), "pre_up": (pre_up, s_pre_up),
        "pre_down": (pre_down, s_pre_down), "branch": (branch_proj, s_branch),
        "gate": (gate_proj, s_gate), "out": (out_proj, s_out),
        "post_gate": (post_gate, s_post_gate), "post_up": (post_up, s_post_up),
        "post_down": (post_down, s_post_down),
        "pre_gain": (h_pre_gain, pre_gain), "mix_gain": (h_mix_gain, mix_gain),
        "channel_gain": (h_channel_gain, channel_gain), "post_gain": (h_post_gain, post_gain),
        "taps": (h_taps, taps), "retain": (h_retain, retain), "admit": (h_admit, admit), "decay": (h_decay, decay),
    }
    loads = {}
    for n, (key, (src, dst)) in enumerate(shards.items()):
        loads[key] = pltpu.make_async_copy(src, dst, local_sem.at[n])
        loads[key].start()
    loads["tokens"] = pltpu.make_async_copy(tokens, x1.at[me], local_sem.at[len(shards)])
    loads["tokens"].start()

    def loaded(*keys):
        for key in keys:
            if key in loads:
                loads.pop(key).wait()

    def toward(axis, n, index, distance):
        return {axis: lax.rem(index + distance + n, n)}

    neighbours = [toward(a, n, i, d) for a, n, i in (("z", NZ, z), ("x", NX, x), ("y", NY, y)) for d in (1, -1)]
    neighbours.append({"c": 1 - c})
    barrier = pltpu.get_barrier_semaphore()
    for device in neighbours:
        pl.semaphore_signal(barrier, inc=1, device_id=device, device_id_type=MESH)

    used = {"recv": 0}
    recv_of, drains = {}, []

    def take():
        used["recv"] += 1
        return sems.at[used["recv"] - 1]

    def receipt(message):
        if message not in recv_of:
            recv_of[message] = take()
        return recv_of[message]

    def send(message, send_sem, ref, device):
        pltpu.make_async_remote_copy(
            src_ref=ref, dst_ref=ref, send_sem=send_sem, recv_sem=receipt(message),
            device_id=device, device_id_type=MESH,
        ).start()

    def await_bytes(ref, sem):
        pltpu.make_async_copy(ref, ref, sem).wait()

    lane = lax.broadcasted_iota(jnp.int32, (352, 384), 1)
    row = lax.broadcasted_iota(jnp.int32, (352, 384), 0)
    group = (lane >= 96).astype(jnp.int32) + (lane >= 192).astype(jnp.int32) + (lane >= 288).astype(jnp.int32)
    spread[...] = jnp.where((row == lane - 8 * group) & (lane - 96 * group < 88), 1.0, 0.0).astype(BF16)

    def put(name, tile, value):
        start = OFFSET[name] + UNIT[name] * tile
        slab[z, x, start : start + UNIT[name], :] = value.astype(BF16)

    def build_wide(name, gate_key, up_key):
        for half, key in enumerate((gate_key, up_key)):
            loaded(key)
            placed = jnp.dot(shards[key][1][...].astype(BF16), spread[...], preferred_element_type=F32)
            for tile in range(3):
                put(name, half + 2 * tile, placed[:, tile * LANES : (tile + 1) * LANES])

    def build_down(name, key):
        loaded(key)
        for tile in range(2):
            value = shards[key][1][:, tile * LANES : (tile + 1) * LANES]
            put(name, tile, jnp.concatenate((value, jnp.zeros((8, LANES), F32)), axis=0))

    def build_mixer():
        loaded("branch")
        put(W3, 0, s_branch[...])
        loaded("gate")
        put(W3, 1, s_gate[...])

    def build_out():
        loaded("out")
        for tile in range(2):
            put(W4, tile, s_out[:, tile * LANES : (tile + 1) * LANES])

    def build_blocks():
        loaded("retain", "admit")
        tall = lax.broadcasted_iota(jnp.int32, (LANES, 64), 0)
        flat = lax.broadcasted_iota(jnp.int32, (LANES, 64), 1)
        wide_r = lax.broadcasted_iota(jnp.int32, (64, LANES), 0)
        wide_c = lax.broadcasted_iota(jnp.int32, (64, LANES), 1)
        for n, ref in enumerate((retain, admit)):
            total = jnp.zeros((LANES, LANES), F32)
            for b in range(2):
                left = jnp.where(tall == flat + 64 * b, 1.0, 0.0).astype(BF16)
                right = jnp.where(wide_c == wide_r + 64 * b, 1.0, 0.0).astype(BF16)
                spread_b = jnp.dot(ref[b].astype(BF16), right, preferred_element_type=F32).astype(BF16)
                total = total + jnp.dot(left, spread_b, preferred_element_type=F32)
            blocks[n] = total.astype(BF16)

    builds = {
        W1: lambda: build_wide(W1, "pre_gate", "pre_up"),
        W2: lambda: build_down(W2, "pre_down"),
        W3: build_mixer,
        W4: build_out,
        W5: lambda: build_wide(W5, "post_gate", "post_up"),
        W6: lambda: build_down(W6, "post_down"),
    }

    tasks = []

    def add(*args, **kwargs):
        tasks.append(Task(*args, **kwargs))

    def ring(label, axis, groups, block, blocks_of, rank, size):
        n, index = {"x": (NX, x), "z": (NZ, z)}[axis]
        far = n // 2
        send_sem = take()
        total = n - 1
        count = sum(len(group) for group in groups)
        drains.append((blocks_of(total, count), send_sem))
        starts = []
        for g, group in enumerate(groups):
            width = len(group)

            def hop(way, k, group=group, g=g):
                sign = step if way == "f" else -step
                origin = lax.rem(index - sign * (k - 1) + n, n)
                for member in group:
                    ref = block(origin, member)
                    send((label, g, k), send_sem, ref, toward(axis, n, index, sign))

            def queued(k, g=g, width=width):
                ways = "fb" if k < far else "f"
                return [((label, g, k, way), axis + way, size * width) for way in ways]

            names = []
            for k in range(1, far + 1):
                def relay(k=k, hop=hop, g=g, width=width):
                    await_bytes(blocks_of(2 if k < far else 1, width), recv_of[(label, g, k)])
                    if k < far:
                        hop("f", k + 1)
                    if k < far - 1:
                        hop("b", k + 1)
                names.append((label, g, k))
                needs = [m for m, _, _ in queued(k)]
                starts_k = relay
                ring_tasks[(label, g, k)] = Task(
                    (label, g, k), relay, after=((label, g, k - 1),), needs=needs, rank=rank,
                    sends=queued(k + 1) if k < far else (), cost=0.03, held=True)

            def begin(hop=hop):
                hop("f", 1)
                hop("b", 1)

            starts.append((begin, queued(1), names))
        return starts

    ring_tasks = {}
    piece_done = {}
    for p, (label, first, rows_a, rows_b, needed, groups_a, groups_b) in enumerate(PIECES):
        for name in needed:
            if not any(task.name == ("build", name) for task in tasks):
                add(("build", name), builds[name], cost=0.4 if name == W5 else 0.1, rank=p)
        span_a, span_b = slice(first, first + rows_a), slice(first + rows_a, first + rows_a + rows_b)
        size_a, size_b = rows_a * LANES * 2, rows_b * LANES * 2

        def bytes_a(ways, width, s=span_a):
            return slab.at[pl.ds(0, ways), pl.ds(0, width), s, :]

        def bytes_b(ways, width, s=span_b):
            return slab.at[pl.ds(0, width), pl.ds(0, ways), s, :]

        def first_ring(part, axis, block, size, blocks_of, second, groups):
            n = {"x": NX, "z": NZ}[axis]
            far = n // 2
            [(begin, queued, names)] = ring((label, part, axis), axis, ((None,),), block, blocks_of, p, size)
            key = (label, part, axis, "start")
            ready = tuple(("build", name) for name in needed) + (("enter",),)
            starters = {}
            for g, group in enumerate(groups):
                starters.setdefault(group[-1], []).append(g)

            def launch(k):
                for g in starters.get(k, ()):
                    second[g][0]()

            def launch_sends(k):
                return [m for g in starters.get(k, ()) for m in second[g][1]]

            def starting():
                begin()
                launch(0)

            add(key, starting, after=ready, rank=p, sends=list(queued) + launch_sends(0), cost=0.04, gate=(GATES[part + label][0], label, GATES[part + label][1]), held=True)
            previous, last = key, None
            for k, name in enumerate(names, 1):
                task = ring_tasks[name]

                def run(inner=task.fn, k=k):
                    inner()
                    launch(k)

                add(name, run, after=(previous,), needs=task.needs, rank=p, cost=0.04, held=True,
                    sends=task.sends + tuple(launch_sends(k)))
                previous = name
            ends = []
            for g, group in enumerate(groups):
                begun = key if group[-1] == 0 else names[group[-1] - 1]
                for k, name in enumerate(second[g][2], 1):
                    task = ring_tasks[name]
                    add(name, task.fn, after=(begun if k == 1 else second[g][2][k - 2],), needs=task.needs,
                        rank=p, sends=task.sends, cost=0.03, held=True)
                ends.append(second[g][2][-1])
            return (previous,) + tuple(ends)

        def members_a(group):
            return tuple(d for k in group for d in ((0,) if k == 0 else (-step, step) if k == 1 else (2,)))

        def members_b(group):
            return tuple(d for k in group for d in ((0,) if k == 0 else (-step * k, step * k) if k < 4 else (4,)))

        second_a = ring(
            (label, "a", "z"), "z", tuple(members_a(g) for g in groups_a),
            lambda i, d, s=span_a: slab.at[i, lax.rem(x + d + NX, NX), s, :], bytes_a, p, size_a)
        second_b = ring(
            (label, "b", "x"), "x", tuple(members_b(g) for g in groups_b),
            lambda i, d, s=span_b: slab.at[lax.rem(z + d + NZ, NZ), i, s, :], bytes_b, p, size_b)
        done_a = first_ring(
            "a", "x", lambda i, _, s=span_a: slab.at[z, i, s, :], size_a, bytes_a, second_a, groups_a)
        done_b = first_ring(
            "b", "z", lambda i, _, s=span_b: slab.at[i, x, s, :], size_b,
            lambda ways, width, s=span_b: slab.at[pl.ds(0, ways), pl.ds(0, width), s, :], second_b, groups_b)
        piece_done[label] = done_a + done_b
        if p:
            for task in tasks:
                if task.name in ((label, "a", "x", "start"), (label, "b", "z", "start")):
                    task.after = task.after + ((PIECES[p - 1][0],) + task.name[1:],)

    held = {1: x1, 2: h1, 3: x2, 4: mixed, 5: x3, 6: h2}
    share_sems = {stage: take() for stage in held}
    for stage, ref in held.items():
        drains.append((ref.at[pl.ds(0, 7)], share_sems[stage]))
    up, down, partner = toward("y", NY, y, step), toward("y", NY, y, -step), {"c": 1 - c}

    def slot_at(distance):
        return lax.rem(y + distance + NY, NY) * 2 + c

    def part_of(stage, unit, slots):
        row, rows, first, lanes = UNITS[stage][unit]
        return held[stage].at[slots, row : row + rows, first : first + lanes]

    def share(stage, unit, slot, hops):
        for tag, device in hops:
            send((stage, unit, tag), share_sems[stage], part_of(stage, unit, slot), device)

    def share_own(stage, unit):
        share(stage, unit, me, (("near", up), ("near", down), ("d", partner)))

    def unit_size(stage, unit):
        return UNITS[stage][unit][1] * UNITS[stage][unit][3] * 2

    def own_sends(stage, unit):
        size = unit_size(stage, unit)
        return [((stage, unit, "f1"), "yf", size), ((stage, unit, "b1"), "yb", size), ((stage, unit, "d0"), "d", size)]

    def share_tasks(stage, unit):
        size = unit_size(stage, unit)

        def first():
            await_bytes(part_of(stage, unit, pl.ds(0, 2)), recv_of[(stage, unit, "near")])
            share(stage, unit, slot_at(-step), (("far", up), ("d", partner)))
            share(stage, unit, slot_at(step), (("d", partner),))

        def second():
            await_bytes(part_of(stage, unit, 0), recv_of[(stage, unit, "far")])
            share(stage, unit, slot_at(2), (("d", partner),))

        add((stage, unit, "first"), first, needs=((stage, unit, "f1"), (stage, unit, "b1")), rank=-2, cost=0.1,
            sends=[((stage, unit, "f2"), "yf", size), ((stage, unit, "d1"), "d", size), ((stage, unit, "d2"), "d", size)])
        add((stage, unit, "second"), second, after=((stage, unit, "first"),), needs=((stage, unit, "f2"),), rank=-2,
            sends=[((stage, unit, "d3"), "d", size)])

    def rows_of(chunk):
        return slice(chunk * SEQ_LEN, (chunk + 1) * SEQ_LEN)

    def weight(name, first, count):
        unit = UNIT[name]
        parts = []
        for tile in range(first, first + count):
            start = OFFSET[name] + unit * tile
            parts.append(slab[:, :, start : start + unit, :].reshape(NZ * NX * unit, LANES))
        return jnp.concatenate(parts, axis=1)

    def normalized(ref, chunk, gain, width, key):
        loaded(key)
        squares = jnp.zeros((SEQ_LEN, LANES), F32)
        for slot in range(TP):
            value = ref[slot, rows_of(chunk), :].astype(F32)
            wide[rows_of(chunk), slot * width : (slot + 1) * width] = (
                value * gain[:, slot * width : (slot + 1) * width]
            ).astype(BF16)
            square = value * value
            for lane_tile in range(width // LANES):
                squares = squares + square[:, lane_tile * LANES : (lane_tile + 1) * LANES]
        mean = jnp.sum(squares, axis=1, keepdims=True) * (1.0 / (TP * width))
        factor = jnp.broadcast_to(lax.rsqrt(mean + EPSILON), (SEQ_LEN, LANES))
        factors[rows_of(chunk), :] = factor
        return factor

    def product(lhs, name, first, count):
        return jnp.dot(lhs, weight(name, first, count), preferred_element_type=F32)

    def up_unit(name, target, unit):
        row, rows, first, lanes = unit
        span = slice(row, row + rows)
        factor = factors[span, :]
        for tile in range(first // LANES, (first + lanes) // LANES):
            both = product(wide[span, :], name, 2 * tile, 2)
            target[me, span, tile * LANES : (tile + 1) * LANES] = (
                silu(both[:, :LANES] * factor) * (both[:, LANES:] * factor)
            ).astype(BF16)

    def down_stage(source, name, residual, finish):
        def run(chunk):
            lhs = jnp.concatenate([source[slot, rows_of(chunk), :] for slot in range(TP)], axis=1)
            total = product(lhs, name, 0, 2)
            finish(chunk, (residual[me, rows_of(chunk), :].astype(F32) + 0.5 * total).astype(BF16))
        return run

    def finish_into(target):
        def finish(chunk, value):
            target[me, rows_of(chunk), :] = value
        return finish

    stores = []

    def finish_out(chunk, value):
        result[rows_of(chunk), :] = value
        stores.append(pltpu.make_async_copy(
            result.at[rows_of(chunk), :], out.at[rows_of(chunk), :], local_sem.at[len(shards) + 1 + chunk]))
        stores[-1].start()

    def mix_stage(chunk):
        factor = normalized(x2, chunk, mix_gain, 256, "mix_gain")
        both = product(wide[rows_of(chunk), :], W3, 0, 2)
        loaded("taps", "decay")
        branch, gate_act = both[:, :LANES] * factor, both[:, LANES:] * factor
        time = lax.broadcasted_iota(jnp.int32, (SEQ_LEN, LANES), 0)

        def earlier(value, k, fill):
            return jnp.where(time >= k, pltpu.roll(value, k, 0), fill)

        convolved = jnp.zeros((SEQ_LEN, LANES), F32)
        for k in range(4):
            lag = 3 - k
            shifted = branch if lag == 0 else earlier(branch, lag, 0.0)
            convolved = convolved + shifted * taps[k : k + 1, :]
        convolved = convolved.astype(BF16)
        retained = sigmoid(jnp.dot(convolved, blocks[0], preferred_element_type=F32))
        admitted = sigmoid(jnp.dot(convolved, blocks[1], preferred_element_type=F32))
        rate = DECAY_SCALE * softplus(-decay[...]) * retained
        add_now = jnp.sqrt(stable_one_minus_exp(2.0 * rate)) * admitted * convolved.astype(F32)
        keep = jnp.exp(-rate)
        k = 1
        while k < SEQ_LEN:
            add_now = keep * earlier(add_now, k, 0.0) + add_now
            if 2 * k < SEQ_LEN:
                keep = keep * earlier(keep, k, 1.0)
            k *= 2
        mixed[me, rows_of(chunk), :] = (add_now * gelu(gate_act)).astype(BF16)

    def out_stage(chunk):
        factor = normalized(mixed, chunk, channel_gain, 128, "channel_gain")
        total = product(wide[rows_of(chunk), : TP * LANES], W4, 0, 2) * jnp.concatenate((factor, factor), axis=1)
        x3[me, rows_of(chunk), :] = (x2[me, rows_of(chunk), :].astype(F32) + total).astype(BF16)

    def enter():
        loaded("tokens")
        pl.semaphore_wait(barrier, len(neighbours))

    add(("enter",), enter, after=(("build", W1),), rank=-5)
    add(("build", "blocks"), build_blocks, cost=0.3, rank=3, after=(("enter",),))
    first_sends = ((PIECES[0][0], "a", "x", "start"), (PIECES[0][0], "b", "z", "start"))
    for task in tasks:
        if task.name[0] == "build" and task.name[1] != W1:
            task.after = task.after + first_sends
    for unit in range(len(UNITS[1])):
        add(("share", 1, unit), functools.partial(share_own, 1, unit), after=first_sends, sends=own_sends(1, unit), rank=1)
    for stage in held:
        for unit in range(len(UNITS[stage])):
            share_tasks(stage, unit)

    def inputs(stage, chunk):
        row = chunk * SEQ_LEN
        units = [u for u, (r, n, _, _) in enumerate(UNITS[stage]) if r <= row < r + n]
        return units, [(stage, u, "d%d" % n) for u in units for n in range(4)], [(stage, u, "second") for u in units]

    received = set()

    def receive(stage, chunk):
        for unit in inputs(stage, chunk)[0]:
            if (stage, unit) not in received:
                received.add((stage, unit))
                await_bytes(part_of(stage, unit, pl.ds(0, 4)), recv_of[(stage, unit, "d")])

    def add_up(stage, source, gain, name, target, labels):
        for chunk in range(CHUNKS):
            def norm(chunk=chunk):
                receive(stage, chunk)
                normalized(source, chunk, gain, 256, "pre_gain" if stage == 1 else "post_gain")
            _, needs, after = inputs(stage, chunk)
            if stage == 5:
                after = after + [("compute", 4, n) for n in range(CHUNKS)]
            add(("norm", stage, chunk), norm, after=after, needs=needs, cost=COST["norm"], rank=2)
        for u, unit in enumerate(UNITS[stage + 1]):
            row, rows, first, lanes = unit
            def run(u=u, unit=unit):
                up_unit(name, target, unit)
                share_own(stage + 1, u)
            pieces = labels[first // LANES : (first + lanes) // LANES]
            after = [t for piece in pieces for t in piece_done[piece]]
            after += [("norm", stage, n) for n in range(row // SEQ_LEN, (row + rows) // SEQ_LEN)]
            add(("tile", stage, u), run, after=after, sends=own_sends(stage + 1, u), rank=-1,
                cost=COST["tile"] * (1.0 + rows * lanes / (SEQ_LEN * LANES)))

    def add_rows(stage, run, piece, before=()):
        for chunk in range(CHUNKS):
            def compute(chunk=chunk):
                receive(stage, chunk)
                run(chunk)
                if stage < 6:
                    share_own(stage + 1, chunk)
            _, needs, after = inputs(stage, chunk)
            after = after + list(piece_done[piece]) + list(before(chunk) if before else ())
            add(("compute", stage, chunk), compute, after=after, needs=needs, rank=-1, cost=COST[stage],
                sends=own_sends(stage + 1, chunk) if stage < 6 else ())

    add_up(1, x1, pre_gain, W1, h1, ("1a", "1b", "1c"))
    add_rows(2, down_stage(h1, W2, x1, finish_into(x2)), "2")
    add_rows(3, mix_stage, "34", lambda chunk: [("build", "blocks")] + [("tile", 1, u) for u in range(len(UNITS[2]))])
    add_rows(4, out_stage, "34")
    add_up(5, x3, post_gain, W5, h2, ("5", "5", "5"))
    add_rows(6, down_stage(h2, W6, x3, finish_out), "6")

    for task in ordered(tasks):
        task.fn()
    for ref, sem in drains:
        await_bytes(ref, sem)
    for store in stores:
        store.wait()
    assert used["recv"] <= SEMS, used["recv"]


def layer(
    tokens, pre_gain, pre_gate, pre_up, pre_down, mix_gain, branch_proj, gate_proj, conv_taps,
    retain_blocks, admit_blocks, decay_param, channel_gain, out_proj, post_gain, post_gate,
    post_up, post_down,
):
    large = (tokens, pre_gate, pre_up, pre_down, branch_proj, gate_proj, out_proj, post_gate, post_up, post_down)
    small = (
        pre_gain.reshape(1, -1), mix_gain.reshape(1, -1), channel_gain.reshape(1, -1),
        post_gain.reshape(1, -1), conv_taps, retain_blocks, admit_blocks, decay_param.reshape(1, -1),
    )
    return pl.pallas_call(
        kernel,
        out_shape=jax.ShapeDtypeStruct(tokens.shape, tokens.dtype),
        in_specs=[pl.BlockSpec(memory_space=pl.ANY)] * (len(large) + len(small)),
        out_specs=pl.BlockSpec(memory_space=pl.ANY),
        scratch_shapes=[pltpu.VMEM(a.shape, F32) for a in large[1:] + small]
        + [
            pltpu.VMEM(tokens.shape, BF16),
            pltpu.VMEM((NZ, NX, SLAB, LANES), BF16),
            pltpu.VMEM((TP, ROWS, 256), BF16),
            pltpu.VMEM((TP, ROWS, 256), BF16),
            pltpu.VMEM((TP, ROWS, 256), BF16),
            pltpu.VMEM((TP, ROWS, 384), BF16),
            pltpu.VMEM((TP, ROWS, 384), BF16),
            pltpu.VMEM((TP, ROWS, 128), BF16),
            pltpu.VMEM((ROWS, 2048), BF16),
            pltpu.VMEM((ROWS, LANES), F32),
            pltpu.VMEM((352, 384), BF16),
            pltpu.VMEM((2, LANES, LANES), BF16),
            pltpu.SemaphoreType.DMA((len(large) + len(small) + CHUNKS,)),
            pltpu.SemaphoreType.DMA((SEMS,)),
        ],
        compiler_params=pltpu.CompilerParams(
            collective_id=0, has_side_effects=True, vmem_limit_bytes=56 * 1024 * 1024
        ),
        name="layer",
    )(*large, *small)


def solution(mesh):
    torus = Mesh(mesh.devices.reshape(NZ, NX, NY, 2), ("z", "x", "y", "c"))
    fs, tp = ("z", "x"), ("y", "c")
    split = P(fs, tp)
    placed = (
        split, P(), split, split, split, P(), split, split, P(None, tp), P(tp, None, None),
        P(tp, None, None), P(tp), P(), split, P(), split, split, split,
    )
    return jax.shard_map(layer, mesh=torus, in_specs=placed, out_specs=split, check_vma=False)
```
